32 devices in a mesh: sp: 4 (over z), dp: 8 (over y, x, core).
Axes of the slice: x: 2, y: 2, z: 4, core: 2. Of those that a mesh axis runs over, the one named last changes fastest.
Arguments:
- queries: bfloat16 [8, 768, 6144], P('dp', None, 'sp'), may hold values from -64 to 64
- out_grad: bfloat16 [8, 768, 4096], P('dp', None, 'sp'), may hold values from -6 to 6
- latent: bfloat16 [8, 768, 512], P('dp'), may hold values from -6 to 6
- rope_key: bfloat16 [8, 768, 64], P('dp'), may hold values from -6 to 6
- kv_gain: float32 [512], replicated, may hold values from 0.1 to 1.9
- key_up: bfloat16 [512, 4096], P('dp', 'sp'), may hold values from -0.25 to 0.25
- value_up: bfloat16 [512, 4096], P('dp', 'sp'), may hold values from -0.25 to 0.25
Outputs:
- query_grad: bfloat16 [8, 768, 6144], P('dp', None, 'sp')
- latent_grad: bfloat16 [8, 768, 512], P('dp')
- rope_key_grad: bfloat16 [8, 768, 64], P('dp')
- key_up_grad: float32 [512, 4096], P('dp', 'sp')
- value_up_grad: float32 [512, 4096], P('dp', 'sp')
The draws below stay inside these ranges and needn't reach their ends.
All inputs are finite; a program needn't handle non-finite values.
Results may differ from the reference program's by a relative error of at most 0.019.
The reference program's roundings to bfloat16 on the way count: a program that leaves them out, or rounds other values in their place, can miss the bound.
Values may be sent and summed in bfloat16 or wider, within the bound.
No kernel may reach another device: no remote copies, remote signals or barrier semaphores. Data moves between devices by JAX's collectives and lax.ppermute only.
A program may use at most 64 MiB of HBM per device.

```python
import jax
import jax.numpy as jnp
from jax import lax

HEADS = 32
NOPE_DIM = 128
ROPE_DIM = 64
VALUE_DIM = 128
LATENT = 512
SEQ_LEN = 768
BATCH = 8
TOKENS = 6144
N_SP = 4


def draw_queries(key, part):
    shape = (BATCH, SEQ_LEN, HEADS * (NOPE_DIM + ROPE_DIM))
    base_key = jax.random.fold_in(key, 0)
    entries = jnp.clip(jax.random.normal(base_key, shape, jnp.float32), -6.0, 6.0)
    return entries.astype(jnp.bfloat16)


def shard_levels(stream_key, dims, pieces, smallest, high):
    level, own = 1.0, jax.random.fold_in(stream_key, 6)
    for dim, blocks in pieces:
        steps = jnp.exp(jax.random.uniform(jax.random.fold_in(own, dim), (blocks,), jnp.float32, smallest / len(pieces), high / len(pieces)))
        level = level * jnp.repeat(steps, dims[dim] // blocks).reshape([-1 if axis == dim else 1 for axis in range(len(dims))])
    return level


def normal_values(own_key, extent, scale, limit, shards=(), kind=jnp.bfloat16):
    result = jax.random.normal(own_key, extent, jnp.float32) * scale
    if len(shards) > 0:
        result = shard_levels(own_key, extent, shards, -0.22, 0.18) * result
    return jnp.clip(result, min=-limit, max=limit).astype(kind)


def setup_inputs(seed: int = 0) -> dict:
    splits = jax.random.split(jax.random.key(seed), 8)
    queries = draw_queries(jax.random.fold_in(splits[7], 71), 0)
    out_grad = normal_values(splits[1], (BATCH, SEQ_LEN, HEADS * VALUE_DIM), 1.0, 6.0, ((0, 8), (2, 4)))
    latent = normal_values(splits[2], (BATCH, SEQ_LEN, LATENT), 1.0, 6.0, ((0, 8),))
    rope_key = normal_values(splits[3], (BATCH, SEQ_LEN, ROPE_DIM), 1.0, 6.0, ((0, 8),))
    kv_gain = jnp.clip(1.0 + 0.18 * jax.random.normal(splits[4], (LATENT,), jnp.float32), 0.1, 1.9)
    key_up = normal_values(splits[5], (LATENT, HEADS * NOPE_DIM), LATENT ** -0.5, 0.25, ((0, 8), (1, 4)))
    value_up = normal_values(splits[6], (LATENT, HEADS * VALUE_DIM), LATENT ** -0.5, 0.25, ((0, 8), (1, 4)))
    return {"queries": queries, "out_grad": out_grad, "latent": latent, "rope_key": rope_key, "kv_gain": kv_gain, "key_up": key_up, "value_up": value_up}


norm_eps = 1e-06
rope_theta = 10000.0

def rope_tables(length, width):
    half_width = width // 2
    frequency = rope_theta ** (-(jnp.arange(half_width, dtype=jnp.float32) * 2.0 / width))
    position = jnp.arange(length, dtype=jnp.int32).astype(jnp.float32)
    angles = position[:, None] * frequency[None, :]
    return (jnp.cos(angles), jnp.sin(angles))

def rotate(tensor, cosine, sine_table):
    half_width = tensor.shape[-1] // 2
    first_half = tensor[..., :half_width]
    second = tensor[..., half_width:]
    return jnp.concatenate([first_half * cosine - second * sine_table, second * cosine + first_half * sine_table], axis=-1)

def unrotate(upstream, cosine, sine_table):
    half_width = upstream.shape[-1] // 2
    first_half = upstream[..., :half_width]
    second = upstream[..., half_width:]
    return jnp.concatenate([first_half * cosine + second * sine_table, second * cosine - first_half * sine_table], axis=-1)

def head_backward(query_used, key_used, head_value, head_grad, score_scale):
    length = query_used.shape[0]
    scores = jnp.dot(query_used, key_used.T, preferred_element_type=jnp.float32) * score_scale
    causal = lax.broadcasted_iota(jnp.int32, (length, length), 0) >= lax.broadcasted_iota(jnp.int32, (length, length), 1)
    scores = jnp.where(causal, scores, -jnp.inf)
    row_top = lax.optimization_barrier(jnp.max(scores, axis=1, keepdims=True))
    weights = jnp.exp(scores - row_top)
    probs = weights / lax.optimization_barrier(jnp.sum(weights, axis=1, keepdims=True))
    probs_low = probs.astype(jnp.bfloat16)
    value_grad = jnp.dot(probs_low.T, head_grad, preferred_element_type=jnp.float32).astype(jnp.bfloat16)
    prob_grad = jnp.dot(head_grad, head_value.T, preferred_element_type=jnp.float32)
    center = lax.optimization_barrier(jnp.sum(probs * prob_grad, axis=1, keepdims=True))
    score_grad = (probs * (prob_grad - center) * score_scale).astype(jnp.bfloat16)
    query_grad = jnp.dot(score_grad, key_used, preferred_element_type=jnp.float32)
    key_grad = jnp.dot(score_grad.T, query_used, preferred_element_type=jnp.float32)
    return (query_grad, key_grad, value_grad)

def attend(queries, head_grads, keys, values, key_rot, cosine, sine_table):
    length = queries.shape[0]
    head_count = head_grads.shape[1] // VALUE_DIM
    qk_width = NOPE_DIM + ROPE_DIM
    query_heads = queries.reshape(length, head_count, qk_width)
    rotated = rotate(query_heads[:, :, NOPE_DIM:].astype(jnp.float32), cosine[:, None, :], sine_table[:, None, :]).astype(jnp.bfloat16)
    query_used = jnp.concatenate([query_heads[:, :, :NOPE_DIM], rotated], axis=-1).transpose(1, 0, 2)
    key_heads = keys.reshape(length, head_count, NOPE_DIM).transpose(1, 0, 2)
    key_used = jnp.concatenate([key_heads, jnp.broadcast_to(key_rot[None], (head_count, length, ROPE_DIM))], axis=-1)
    value_heads = values.reshape(length, head_count, VALUE_DIM).transpose(1, 0, 2)
    grad_heads = head_grads.reshape(length, head_count, VALUE_DIM).transpose(1, 0, 2)
    score_scale = qk_width ** (-0.5)
    query_part, key_part, value_part = lax.map(lambda items: head_backward(items[0], items[1], items[2], items[3], score_scale), (query_used, key_used, value_heads, grad_heads))
    query_rot_grad = unrotate(query_part[:, :, NOPE_DIM:], cosine[None], sine_table[None])
    query_grad = jnp.concatenate([query_part[:, :, :NOPE_DIM], query_rot_grad], axis=-1).astype(jnp.bfloat16)
    query_grad = query_grad.transpose(1, 0, 2).reshape(length, head_count * qk_width)
    key_plain_grad = key_part[:, :, :NOPE_DIM].astype(jnp.bfloat16).transpose(1, 0, 2).reshape(length, head_count * NOPE_DIM)
    key_rot_grad = lax.optimization_barrier(jnp.sum(key_part[:, :, NOPE_DIM:], axis=0))
    value_grad = value_part.transpose(1, 0, 2).reshape(length, head_count * VALUE_DIM)
    return (query_grad, key_plain_grad, key_rot_grad, value_grad)

def finish(comp_total, rot_total, raw_latent, inverse, kv_gain, cosine, sine_table):
    mixed = comp_total * kv_gain
    spread = lax.optimization_barrier(jnp.mean(raw_latent * mixed, axis=-1, keepdims=True))
    latent_grad = (inverse * mixed - raw_latent * inverse ** 3 * spread).astype(jnp.bfloat16)
    rope_grad = unrotate(rot_total, cosine, sine_table).astype(jnp.bfloat16)
    return (latent_grad, rope_grad)

def reference(queries, out_grad, latent, rope_key, kv_gain, key_up, value_up):
    qk_width = NOPE_DIM + ROPE_DIM
    group = HEADS // N_SP
    cosine, sine_table = rope_tables(SEQ_LEN, ROPE_DIM)

    def one_sequence(totals, inputs):
        key_total, value_total = totals
        seq_queries, seq_grad, seq_latent, seq_rope = inputs
        raw_latent = seq_latent.astype(jnp.float32)
        inverse = lax.rsqrt(lax.optimization_barrier(jnp.mean(raw_latent * raw_latent, axis=-1, keepdims=True)) + norm_eps)
        compressed = (raw_latent * inverse * kv_gain).astype(jnp.bfloat16)
        key_rot = rotate(seq_rope.astype(jnp.float32), cosine, sine_table).astype(jnp.bfloat16)
        keys = jnp.dot(compressed, key_up, preferred_element_type=jnp.float32).astype(jnp.bfloat16)
        values = jnp.dot(compressed, value_up, preferred_element_type=jnp.float32).astype(jnp.bfloat16)

        def per_group(index):
            query_cols = lax.dynamic_slice_in_dim(seq_queries, index * (group * qk_width), group * qk_width, 1)
            grad_cols = lax.dynamic_slice_in_dim(seq_grad, index * (group * VALUE_DIM), group * VALUE_DIM, 1)
            key_cols = lax.dynamic_slice_in_dim(keys, index * (group * NOPE_DIM), group * NOPE_DIM, 1)
            value_cols = lax.dynamic_slice_in_dim(values, index * (group * VALUE_DIM), group * VALUE_DIM, 1)
            key_weight = lax.dynamic_slice_in_dim(key_up, index * (group * NOPE_DIM), group * NOPE_DIM, 1)
            value_weight = lax.dynamic_slice_in_dim(value_up, index * (group * VALUE_DIM), group * VALUE_DIM, 1)
            query_grad, key_plain_grad, key_rot_grad, value_grad = attend(query_cols, grad_cols, key_cols, value_cols, key_rot, cosine, sine_table)
            comp_part = jnp.dot(key_plain_grad, key_weight.T, preferred_element_type=jnp.float32) + jnp.dot(value_grad, value_weight.T, preferred_element_type=jnp.float32)
            return (query_grad, key_plain_grad, value_grad, comp_part, key_rot_grad)
        query_groups, key_groups, value_groups, comp_parts, rot_parts = lax.map(per_group, jnp.arange(N_SP, dtype=jnp.int32))
        query_grad = query_groups.transpose(1, 0, 2).reshape(SEQ_LEN, HEADS * qk_width)
        key_plain_all = key_groups.transpose(1, 0, 2).reshape(SEQ_LEN, HEADS * NOPE_DIM)
        value_all = value_groups.transpose(1, 0, 2).reshape(SEQ_LEN, HEADS * VALUE_DIM)
        comp_low = lax.optimization_barrier(comp_parts.astype(jnp.bfloat16))
        rot_low = lax.optimization_barrier(rot_parts.astype(jnp.bfloat16))
        comp_total = lax.optimization_barrier(jnp.sum(comp_low.astype(jnp.float32), axis=0))
        rot_total = lax.optimization_barrier(jnp.sum(rot_low.astype(jnp.float32), axis=0))
        latent_grad, rope_grad = finish(comp_total, rot_total, raw_latent, inverse, kv_gain, cosine, sine_table)
        contract = (((0,), (0,)), ((), ()))
        key_total = key_total + lax.dot_general(compressed, key_plain_all, contract, preferred_element_type=jnp.float32)
        value_total = value_total + lax.dot_general(compressed, value_all, contract, preferred_element_type=jnp.float32)
        return ((key_total, value_total), (query_grad, latent_grad, rope_grad))
    start_totals = (jnp.zeros((LATENT, HEADS * NOPE_DIM), jnp.float32), jnp.zeros((LATENT, HEADS * VALUE_DIM), jnp.float32))
    totals, outputs = lax.scan(one_sequence, start_totals, (queries, out_grad, latent, rope_key))
    grad_scale = float(TOKENS) ** (-0.5)
    return (outputs[0], outputs[1], outputs[2], totals[0] * grad_scale, totals[1] * grad_scale)
```

```python
import functools
import math

import jax
import jax.numpy as jnp
from jax import lax
from jax.experimental import pallas as pl
from jax.experimental.pallas import tpu as pltpu
from jax.sharding import PartitionSpec as P

NOPE = 128
ROPE = 64
VALUE = 128
QK = NOPE + ROPE
WIDE = 256
NORM_EPS = 1e-06
THETA = 10000.0
BF = jnp.bfloat16
F32 = jnp.float32
VMEM_LIMIT = 56 * 1024 * 1024


def mm(a, b):
    return jnp.dot(a, b, preferred_element_type=F32)


def turn(upper, lower, cosine, sine):
    return upper * cosine - lower * sine, lower * cosine + upper * sine


def prep_kernel(
    q_ref, do_ref, lat_ref, rope_ref, gain_ref, perm_ref, cos_ref, sin_ref,
    q_out, qt_out, dot_out, comp_out, compt_out, krot_out, krott_out,
):
    length = q_ref.shape[0]
    half = ROPE // 2
    cosine, sine = cos_ref[...], sin_ref[...]

    @pl.when(pl.program_id(0) == 0)
    def _():
        raw = lat_ref[...].astype(F32)
        inverse = lax.rsqrt(jnp.mean(raw * raw, axis=1, keepdims=True) + NORM_EPS)
        comp = (raw * inverse * gain_ref[...]).astype(BF)
        rel = mm(comp, perm_ref[...]).astype(BF)
        comp_out[...] = rel
        compt_out[...] = rel.T
        key_t = rope_ref[...].astype(F32).T
        first, second = turn(key_t[:half], key_t[half:], cosine, sine)
        krot_t = jnp.concatenate([first, second, jnp.zeros_like(key_t)], axis=0).astype(BF)
        krott_out[...] = krot_t
        krot_out[...] = krot_t.T

    q_t = q_ref[...].T
    for h in range(2):
        base = h * QK
        rot = q_t[base + NOPE : base + QK].astype(F32)
        first, second = turn(rot[:half], rot[half:], cosine, sine)
        used = jnp.concatenate(
            [
                q_t[base : base + NOPE],
                first.astype(BF),
                second.astype(BF),
                jnp.zeros((WIDE - QK, length), BF),
            ],
            axis=0,
        )
        qt_out[h] = used
        q_out[h] = used.T
    dot_out[...] = do_ref[...].T


def prep(queries, out_grad, latent, rope_key, gain, perm, cos_t, sin_t):
    length = queries.shape[0]
    heads = out_grad.shape[1] // VALUE
    width = latent.shape[1]
    whole = lambda *shape: pl.BlockSpec(shape, lambda p: (0,) * len(shape))
    return pl.pallas_call(
        prep_kernel,
        grid=(heads // 2,),
        in_specs=[
            pl.BlockSpec((length, 2 * QK), lambda p: (0, p)),
            pl.BlockSpec((length, 2 * VALUE), lambda p: (0, p)),
            whole(length, width),
            whole(length, ROPE),
            whole(1, width),
            whole(width, width),
            whole(ROPE // 2, length),
            whole(ROPE // 2, length),
        ],
        out_specs=[
            pl.BlockSpec((2, length, WIDE), lambda p: (p, 0, 0)),
            pl.BlockSpec((2, WIDE, length), lambda p: (p, 0, 0)),
            pl.BlockSpec((2 * VALUE, length), lambda p: (p, 0)),
            whole(length, width),
            whole(width, length),
            whole(length, 2 * ROPE),
            whole(2 * ROPE, length),
        ],
        out_shape=[
            jax.ShapeDtypeStruct((heads, length, WIDE), BF),
            jax.ShapeDtypeStruct((heads, WIDE, length), BF),
            jax.ShapeDtypeStruct((heads * VALUE, length), BF),
            jax.ShapeDtypeStruct((length, width), BF),
            jax.ShapeDtypeStruct((width, length), BF),
            jax.ShapeDtypeStruct((length, 2 * ROPE), BF),
            jax.ShapeDtypeStruct((2 * ROPE, length), BF),
        ],
        compiler_params=pltpu.CompilerParams(vmem_limit_bytes=VMEM_LIMIT),
        name="prep",
    )(queries, out_grad, latent, rope_key, gain, perm, cos_t, sin_t)


def panel(kext, v, q_t, do_t, scale):
    size = q_t.shape[1]
    span = kext.shape[0]
    scores = mm(kext, q_t)
    grad = mm(v, do_t)
    keep = lax.broadcasted_iota(jnp.int32, (size, size), 0) <= lax.broadcasted_iota(
        jnp.int32, (size, size), 1
    )
    tail = jnp.where(keep, scores[span - size :], -jnp.inf)
    if span > size:
        scores = jnp.concatenate([scores[: span - size], tail], axis=0)
    else:
        scores = tail
    top = jnp.max(scores, axis=0, keepdims=True)
    weights = jnp.exp2((scores - top) * (scale * math.log2(math.e)))
    norm = 1.0 / jnp.sum(weights, axis=0, keepdims=True)
    probs = weights * norm
    center = jnp.sum(probs * grad, axis=0, keepdims=True)
    score_grad = (probs * (grad - center) * scale).astype(BF)
    return probs.astype(BF), score_grad


def query_out(parts, cosine, sine):
    half = ROPE // 2
    rows = []
    for part in parts:
        first, second = part[NOPE : NOPE + half], part[NOPE + half : QK]
        back_first = first * cosine + second * sine
        back_second = second * cosine - first * sine
        rows += [part[:NOPE].astype(BF), back_first.astype(BF), back_second.astype(BF)]
    return jnp.concatenate(rows, axis=0).T


def last_kernel(
    comp_ref, kw_ref, vw_ref, krot_ref, krott_ref, q_ref, qt_ref, do_ref, dot_ref, cos_ref, sin_ref,
    kext_out, kextt_out, v_out, probs_out, grad_out, dq_out, dk_out, dv_out, part_out,
    acc, rot_acc, *, scale, size,
):
    step = pl.program_id(0)
    comp = comp_ref[...]
    length = comp.shape[0]
    before = length - size
    keys = mm(comp, kw_ref[...]).astype(BF)
    values = mm(comp, vw_ref[...]).astype(BF)
    v_out[...] = values[:before]
    dq_parts, dks, dvs = [], [], []
    rot = None
    for h in range(2):
        key = keys[:, h * NOPE : (h + 1) * NOPE]
        value = values[:, h * VALUE : (h + 1) * VALUE]
        kext = jnp.concatenate([key, krot_ref[...]], axis=1)
        kext_t = jnp.concatenate([key.T, krott_ref[...]], axis=0)
        kext_out[h] = kext[:before]
        kextt_out[h] = kext_t[:, :before]
        probs, score_grad = panel(
            kext, value, qt_ref[h], dot_ref[h * VALUE : (h + 1) * VALUE], scale
        )
        probs_out[h] = probs[:before]
        grad_out[h] = score_grad[:before]
        dq_parts.append(mm(kext_t, score_grad))
        dk = mm(score_grad[before:], q_ref[h])
        dvs.append(mm(probs[before:], do_ref[:, h * VALUE : (h + 1) * VALUE]).astype(BF))
        dks.append(dk[:, :NOPE].astype(BF))
        rot = dk[:, NOPE:] if rot is None else rot + dk[:, NOPE:]
    dq_out[...] = query_out(dq_parts, cos_ref[...], sin_ref[...])
    dk_pair = jnp.concatenate(dks, axis=1)
    dv_pair = jnp.concatenate(dvs, axis=1)
    dk_out[...] = dk_pair
    dv_out[...] = dv_pair
    part = mm(dk_pair, kw_ref[...].T) + mm(dv_pair, vw_ref[...].T)

    @pl.when(step == 0)
    def _():
        acc[...] = part
        rot_acc[...] = rot

    @pl.when(step > 0)
    def _():
        acc[...] += part
        rot_acc[...] += rot

    @pl.when(step == pl.num_programs(0) - 1)
    def _():
        part_out[:, : acc.shape[1]] = acc[...].astype(BF)
        part_out[:, acc.shape[1] :] = rot_acc[...].astype(BF)


def run_last(comp, kw, vw, krot, krot_t, q, q_t, do, do_t, cos_t, sin_t, size):
    length, width = comp.shape
    heads = q.shape[0]
    before = length - size
    blk = length // size - 1
    whole = lambda *shape: pl.BlockSpec(shape, lambda p: (0,) * len(shape))
    pair = 2 * NOPE
    return pl.pallas_call(
        functools.partial(last_kernel, scale=QK**-0.5, size=size),
        grid=(heads // 2,),
        in_specs=[
            whole(length, width),
            pl.BlockSpec((width, pair), lambda p: (0, p)),
            pl.BlockSpec((width, pair), lambda p: (0, p)),
            whole(length, 2 * ROPE),
            whole(2 * ROPE, length),
            pl.BlockSpec((2, size, WIDE), lambda p: (p, blk, 0)),
            pl.BlockSpec((2, WIDE, size), lambda p: (p, 0, blk)),
            pl.BlockSpec((size, pair), lambda p: (blk, p)),
            pl.BlockSpec((pair, size), lambda p: (p, blk)),
            pl.BlockSpec((ROPE // 2, size), lambda p: (0, blk)),
            pl.BlockSpec((ROPE // 2, size), lambda p: (0, blk)),
        ],
        out_specs=[
            pl.BlockSpec((2, before, WIDE), lambda p: (p, 0, 0)),
            pl.BlockSpec((2, WIDE, before), lambda p: (p, 0, 0)),
            pl.BlockSpec((before, pair), lambda p: (0, p)),
            pl.BlockSpec((2, before, size), lambda p: (p, 0, 0)),
            pl.BlockSpec((2, before, size), lambda p: (p, 0, 0)),
            pl.BlockSpec((size, 2 * QK), lambda p: (0, p)),
            pl.BlockSpec((size, pair), lambda p: (0, p)),
            pl.BlockSpec((size, pair), lambda p: (0, p)),
            whole(size, width + WIDE - NOPE),
        ],
        out_shape=[
            jax.ShapeDtypeStruct((heads, before, WIDE), BF),
            jax.ShapeDtypeStruct((heads, WIDE, before), BF),
            jax.ShapeDtypeStruct((before, heads * VALUE), BF),
            jax.ShapeDtypeStruct((heads, before, size), BF),
            jax.ShapeDtypeStruct((heads, before, size), BF),
            jax.ShapeDtypeStruct((size, heads * QK), BF),
            jax.ShapeDtypeStruct((size, heads * NOPE), BF),
            jax.ShapeDtypeStruct((size, heads * VALUE), BF),
            jax.ShapeDtypeStruct((size, width + WIDE - NOPE), BF),
        ],
        scratch_shapes=[pltpu.VMEM((size, width), F32), pltpu.VMEM((size, WIDE - NOPE), F32)],
        compiler_params=pltpu.CompilerParams(vmem_limit_bytes=VMEM_LIMIT),
        name="last_block",
    )(comp, kw, vw, krot, krot_t, q, q_t, do, do_t, cos_t, sin_t)


def rest_kernel(
    compt_ref, kw_ref, vw_ref, kext_ref, kextt_ref, v_ref, probs_ref, grad_ref,
    q_ref, qt_ref, do_ref, dot_ref, dk_ref, dv_ref, cos_ref, sin_ref,
    dq_out, kprod_out, vprod_out, part_out, p_all, g_all, acc, rot_acc, *, scale, size, grad_scale,
):
    step = pl.program_id(0)
    before = v_ref.shape[0]
    blocks = before // size
    length = before + size
    rot = [None] * blocks
    dks, dvs = [[] for _ in range(blocks)], [[] for _ in range(blocks)]
    dq_parts = [[] for _ in range(blocks)]
    for h in range(2):
        lanes = slice(h * NOPE, (h + 1) * NOPE)
        p_all[h, :, before:] = probs_ref[h]
        g_all[h, :, before:] = grad_ref[h]
        for b in reversed(range(blocks)):
            end = (b + 1) * size
            cols = slice(b * size, end)
            probs, score_grad = panel(
                kext_ref[h, :end], v_ref[:end, lanes], qt_ref[h, :, cols], dot_ref[lanes, cols], scale
            )
            p_all[h, :end, cols] = probs
            g_all[h, :end, cols] = score_grad
            dq_parts[b].append(mm(kextt_ref[h, :, :end], score_grad))
        for b in range(blocks):
            rows = slice(b * size, (b + 1) * size)
            dk = mm(g_all[h, rows, b * size :], q_ref[h, b * size :])
            dv = mm(p_all[h, rows, b * size :], do_ref[b * size :, lanes])
            dks[b].append(dk[:, :NOPE].astype(BF))
            dvs[b].append(dv.astype(BF))
            rot[b] = dk[:, NOPE:] if h == 0 else rot[b] + dk[:, NOPE:]
    for b in range(blocks):
        cols = slice(b * size, (b + 1) * size)
        dq_out[cols] = query_out(dq_parts[b], cos_ref[:, cols], sin_ref[:, cols])
    dk_pair = jnp.concatenate([jnp.concatenate(d, axis=1) for d in dks], axis=0)
    dv_pair = jnp.concatenate([jnp.concatenate(d, axis=1) for d in dvs], axis=0)
    part = mm(dk_pair, kw_ref[...].T) + mm(dv_pair, vw_ref[...].T)
    rot_part = jnp.concatenate(rot, axis=0)

    @pl.when(step == 0)
    def _():
        acc[...] = part
        rot_acc[...] = rot_part

    @pl.when(step > 0)
    def _():
        acc[...] += part
        rot_acc[...] += rot_part

    comp_t = compt_ref[...]
    kprod = mm(comp_t, jnp.concatenate([dk_pair, dk_ref[...]], axis=0)) * grad_scale
    vprod = mm(comp_t, jnp.concatenate([dv_pair, dv_ref[...]], axis=0)) * grad_scale
    kprod_out[...] = kprod.astype(BF)
    vprod_out[...] = vprod.astype(BF)

    @pl.when(step == pl.num_programs(0) - 1)
    def _():
        part_out[:, : acc.shape[1]] = acc[...].astype(BF)
        part_out[:, acc.shape[1] :] = rot_acc[...].astype(BF)


def run_rest(
    comp_t, kw, vw, kext, kext_t, v, probs, grad, q, q_t, do, do_t, dk, dv, cos_t, sin_t, size, grad_scale
):
    width, length = comp_t.shape
    heads = q.shape[0]
    before = length - size
    whole = lambda *shape: pl.BlockSpec(shape, lambda p: (0,) * len(shape))
    pair = 2 * NOPE
    return pl.pallas_call(
        functools.partial(rest_kernel, scale=QK**-0.5, size=size, grad_scale=grad_scale),
        grid=(heads // 2,),
        in_specs=[
            whole(width, length),
            pl.BlockSpec((width, pair), lambda p: (0, p)),
            pl.BlockSpec((width, pair), lambda p: (0, p)),
            pl.BlockSpec((2, before, WIDE), lambda p: (p, 0, 0)),
            pl.BlockSpec((2, WIDE, before), lambda p: (p, 0, 0)),
            pl.BlockSpec((before, pair), lambda p: (0, p)),
            pl.BlockSpec((2, before, size), lambda p: (p, 0, 0)),
            pl.BlockSpec((2, before, size), lambda p: (p, 0, 0)),
            pl.BlockSpec((2, length, WIDE), lambda p: (p, 0, 0)),
            pl.BlockSpec((2, WIDE, before), lambda p: (p, 0, 0)),
            pl.BlockSpec((length, pair), lambda p: (0, p)),
            pl.BlockSpec((pair, before), lambda p: (p, 0)),
            pl.BlockSpec((size, pair), lambda p: (0, p)),
            pl.BlockSpec((size, pair), lambda p: (0, p)),
            pl.BlockSpec((ROPE // 2, before), lambda p: (0, 0)),
            pl.BlockSpec((ROPE // 2, before), lambda p: (0, 0)),
        ],
        out_specs=[
            pl.BlockSpec((before, 2 * QK), lambda p: (0, p)),
            pl.BlockSpec((width, pair), lambda p: (0, p)),
            pl.BlockSpec((width, pair), lambda p: (0, p)),
            whole(before, width + WIDE - NOPE),
        ],
        out_shape=[
            jax.ShapeDtypeStruct((before, heads * QK), BF),
            jax.ShapeDtypeStruct((width, heads * NOPE), BF),
            jax.ShapeDtypeStruct((width, heads * VALUE), BF),
            jax.ShapeDtypeStruct((before, width + WIDE - NOPE), BF),
        ],
        scratch_shapes=[
            pltpu.VMEM((2, before, length), BF),
            pltpu.VMEM((2, before, length), BF),
            pltpu.VMEM((before, width), F32),
            pltpu.VMEM((before, WIDE - NOPE), F32),
        ],
        compiler_params=pltpu.CompilerParams(vmem_limit_bytes=VMEM_LIMIT),
        name="rest_blocks",
    )(comp_t, kw, vw, kext, kext_t, v, probs, grad, q, q_t, do, do_t, dk, dv, cos_t, sin_t)


def swap(x, axis, mask):
    n = lax.axis_size(axis)
    return lax.ppermute(x, axis, [(i, i ^ mask) for i in range(n)])


def gather_blocks(x, axis, order):
    names, held = [0], x[None]
    for bit in order:
        mask = 1 << bit
        other = swap(held, axis, mask)
        held = jnp.concatenate([held, other], axis=0)
        names = names + [r ^ mask for r in names]
    where = {r: i for i, r in enumerate(names)}
    return jnp.concatenate([held[where[r]] for r in range(len(names))], axis=0)


def scatter_sum(x, axis, order):
    names = list(range(x.shape[0]))
    held = x
    for i, bit in enumerate(order):
        mask = 1 << bit
        kept = [r for r in names if not r & mask]
        sent = [r ^ 0 for r in [k | mask for k in kept]]
        pick = lambda rs: jnp.stack([held[names.index(r)] for r in rs], axis=0)
        got = swap(pick(sent), axis, mask)
        held = pick(kept).astype(F32) + got.astype(F32)
        names = kept
        if i < len(order) - 1:
            held = held.astype(BF)
    return held[0]


def axis_bits(n):
    bits = n.bit_length() - 1
    assert 1 << bits == n
    return bits


def share_rows(x, axis, fn):
    n = lax.axis_size(axis)
    me = lax.axis_index(axis)
    rows = x.shape[0] // n
    take = lambda owner: lax.dynamic_slice_in_dim(x, owner * rows, rows, 0)
    total = take(me).astype(F32)
    for r in range(1, n):
        total = total + swap(take(me ^ r), axis, r).astype(F32)
    mine = fn(total, me * rows, rows)
    out = jnp.zeros((x.shape[0], mine.shape[1]), mine.dtype)
    out = lax.dynamic_update_slice_in_dim(out, mine, me * rows, 0)
    for r in range(1, n):
        out = lax.dynamic_update_slice_in_dim(out, swap(mine, axis, r), (me ^ r) * rows, 0)
    return out


def shards(queries, out_grad, latent, rope_key, kv_gain, key_up, value_up):
    _, length, width = latent.shape
    dp = lax.axis_size("dp")
    size = length // 3
    bits = axis_bits(dp)
    links = list(range(1, bits))
    me = lax.axis_index("dp")
    block = width // dp
    kw = gather_blocks(key_up, "dp", links[::-1] + [0])
    vw = gather_blocks(value_up, "dp", links + [0])

    half = ROPE // 2
    frequency = THETA ** (-(jnp.arange(half, dtype=F32) * 2.0 / ROPE))
    position = jnp.arange(length, dtype=jnp.int32).astype(F32)
    angles = frequency[:, None] * position[None, :]
    cos_t, sin_t = jnp.cos(angles), jnp.sin(angles)
    from_row = lax.broadcasted_iota(jnp.int32, (width, width), 0)
    to_col = lax.broadcasted_iota(jnp.int32, (width, width), 1)
    perm = (from_row == ((to_col // block) ^ me) * block + to_col % block).astype(BF)

    q, do, raw = queries[0], out_grad[0], latent[0]
    q_used, q_t, do_t, comp, comp_t, krot, krot_t = prep(
        q, do, raw, rope_key[0], kv_gain[None], perm, cos_t, sin_t
    )
    kext, kext_t, v, probs, grad, dq_last, dk_last, dv_last, part_last = run_last(
        comp, kw, vw, krot, krot_t, q_used, q_t, do, do_t, cos_t, sin_t, size
    )
    grad_scale = float(dp * length) ** (-0.5)
    dq_rest, kprod, vprod, part_rest = run_rest(
        comp_t, kw, vw, kext, kext_t, v, probs, grad, q_used, q_t, do, do_t,
        dk_last, dv_last, cos_t, sin_t, size, grad_scale,
    )

    def finish_at(offset):
        def finish(total, start, rows):
            lat = lax.dynamic_slice_in_dim(raw, offset + start, rows, 0).astype(F32)
            inverse = lax.rsqrt(jnp.mean(lat * lat, axis=1, keepdims=True) + NORM_EPS)
            latent_total = lax.dot_general(
                total[:, :width], perm.astype(F32), (((1,), (1,)), ((), ())), precision=lax.Precision.HIGHEST,
                preferred_element_type=F32,
            )
            mixed = latent_total * kv_gain
            spread = jnp.mean(lat * mixed, axis=1, keepdims=True)
            latent_grad = (inverse * mixed - lat * inverse**3 * spread).astype(BF)
            cosine = lax.dynamic_slice_in_dim(cos_t, offset + start, rows, 1).T
            sine = lax.dynamic_slice_in_dim(sin_t, offset + start, rows, 1).T
            first, second = total[:, width : width + half], total[:, width + half : width + ROPE]
            rope = jnp.concatenate(
                [first * cosine + second * sine, second * cosine - first * sine], axis=1
            ).astype(BF)
            return jnp.concatenate([latent_grad, rope], axis=1)

        return finish

    done_last = share_rows(part_last, "sp", finish_at(length - size))
    done_rest = share_rows(part_rest, "sp", finish_at(0))
    done = jnp.concatenate([done_rest, done_last], axis=0)
    key_grad = scatter_sum(kprod.reshape(dp, block, -1), "dp", [0] + links)
    value_grad = scatter_sum(vprod.reshape(dp, block, -1), "dp", [0] + links[::-1])
    query_grad = jnp.concatenate([dq_rest, dq_last], axis=0)
    return (
        query_grad[None],
        done[None, :, :width],
        done[None, :, width : width + ROPE],
        key_grad,
        value_grad,
    )


def solution(mesh):
    return jax.shard_map(
        shards,
        mesh=mesh,
        in_specs=(
            P("dp", None, "sp"),
            P("dp", None, "sp"),
            P("dp", None, None),
            P("dp", None, None),
            P(),
            P("dp", "sp"),
            P("dp", "sp"),
        ),
        out_specs=(
            P("dp", None, "sp"),
            P("dp", None, None),
            P("dp", None, None),
            P("dp", "sp"),
            P("dp", "sp"),
        ),
        check_vma=False,
    )
```
